32 devices in a mesh: fs: 8 (over z, y), tp: 4 (over x, core).
Axes of the slice: x: 2, y: 2, z: 4, core: 2. Of those that a mesh axis runs over, the one named last changes fastest.
Arguments:
- cotangent: bfloat16 [5120, 1024], P('fs', 'tp'), may hold values from -6 to 6
- inputs: bfloat16 [5120, 1024], P('fs', 'tp'), may hold values from -6 to 6
- pre_act: bfloat16 [5120, 2112], P('fs'), may hold values from -6 to 6
- w_up: bfloat16 [2112, 1024], P('fs', 'tp'), may hold values from -0.1875 to 0.1875
- w_down: bfloat16 [2112, 1024], P('fs', 'tp'), may hold values from -0.125 to 0.125
Outputs:
- grad_input: bfloat16 [5120, 1024], P('fs', 'tp')
- grad_up: float32 [2112, 1024], P('fs', 'tp')
The draws below stay inside these ranges and needn't reach their ends.
All inputs are finite; a program needn't handle non-finite values.
Results may differ from the reference program's by a relative error of at most 0.0049.
Values may be sent and summed in bfloat16 or wider, within the bound.
A program may use at most 64 MiB of HBM per device.

```python
import jax
import jax.numpy as jnp
from jax import lax

D = 1024
FF = 2112
TOKENS = 5120


def strengthened(drawn, stream_key, source, target, shards_of, factor):
    owner, partner = [(jnp.arange(drawn.shape[position]) // (drawn.shape[position] // shards_of)).reshape([-1 if axis == position else 1 for axis in range(drawn.ndim)]) for position in (source, target)]
    chosen = jax.random.permutation(stream_key, shards_of)[partner]
    strong = (owner == chosen) | (owner == (partner + shards_of // 2) % shards_of)
    return jnp.where(strong, factor * drawn, drawn)


def block_levels(stream_key, shape, pieces, low, largest):
    gain, own = 1.0, jax.random.fold_in(stream_key, 6)
    for dim, parts in pieces:
        draws = jnp.exp(jax.random.uniform(jax.random.fold_in(own, dim), (parts,), jnp.float32, low / len(pieces), largest / len(pieces)))
        gain = gain * jnp.repeat(draws, shape[dim] // parts).reshape([-1 if axis == dim else 1 for axis in range(len(shape))])
    return gain


def bell_draw(key, extent, scale, limit, pieces=(), kind=jnp.bfloat16):
    level = block_levels(key, extent, pieces, -0.22, 0.18) if pieces else 1.0
    result = jax.random.normal(key, extent, jnp.float32) * scale * level
    return jnp.minimum(jnp.maximum(result, -limit), limit).astype(kind)


def gaussian_with(key, shape, deviation, reach, pieces, heavy, kind=jnp.bfloat16):
    drawn = deviation * jax.random.normal(key, shape, jnp.float32)
    if pieces:
        drawn = drawn * block_levels(key, shape, pieces, -0.22, 0.18)
    return jnp.clip(strengthened(drawn, jax.random.fold_in(key, 3), *heavy), -reach, reach).astype(kind)


def setup_inputs(seed: int = 0) -> dict:
    key_of = jax.random.split(jax.random.key(seed), 6)
    return {
        "cotangent": bell_draw(key_of[0], (TOKENS, D), 1.0, 6.0, ((0, 8), (1, 4))),
        "inputs": bell_draw(key_of[1], (TOKENS, D), 1.0, 6.0, ((0, 8), (1, 4))),
        "pre_act": gaussian_with(key_of[2], (TOKENS, FF), 1.0, 6.0, ((0, 8),), (0, 1, 8, 2.0)),
        "w_up": bell_draw(key_of[3], (FF, D), D ** -0.5, 0.1875, ((0, 8), (1, 4))),
        "w_down": bell_draw(key_of[4], (FF, D), FF ** -0.5, 0.125, ((0, 8), (1, 4))),
    }


def reference(cotangent, inputs, pre_act, w_up, w_down):
    grad_hidden = lax.dot_general(cotangent, w_down, (((1,), (1,)), ((), ())), preferred_element_type=jnp.float32)
    grad_pre = (2.0 * grad_hidden * jnp.maximum(pre_act.astype(jnp.float32), 0.0)).astype(jnp.bfloat16)
    grad_input = jnp.dot(grad_pre, w_up, preferred_element_type=jnp.float32).astype(jnp.bfloat16)
    summed = lax.dot_general(grad_pre, inputs, (((0,), (0,)), ((), ())), preferred_element_type=jnp.float32)
    grad_up = summed / jnp.sqrt(jnp.float32(TOKENS))
    return (grad_input, grad_up)
```

```python
import functools

import jax
import jax.numpy as jnp
from jax import lax
from jax.experimental import pallas as pl
from jax.experimental.pallas import tpu as pltpu
from jax.sharding import PartitionSpec as P

MESH = pl.DeviceIdType.MESH
MIDDLE = 8
LAG = 3


def times_rows(left, piece):
    return lax.dot_general(
        left, piece, (((1,), (1,)), ((), ())), preferred_element_type=jnp.float32
    )


def kernel(
    n, token_total,
    cot_hbm, in_hbm, pre_hbm, up_hbm, down_hbm,
    gi_ref, gu_ref,
    cot_buf, cot_turned, in_buf, down_buf, swap_buf, up_buf, pre_buf, grad, held,
    out_buf, in_sum, y_in,
    local_sem, cot_send, cot_recv, swap_send, dz_send, dy_send, dc_send, down_recv,
    uz_send, uy_send, up_recv, gx_send, gx_recv, gc_send, gc_recv,
    rs_send, rs_recv, y_recv,
):
    deep = n // 2
    f = lax.axis_index("fs")
    t = lax.axis_index("tp")
    z, y = f // 2, f % 2
    x, c = t // 2, t % 2
    width = in_buf.shape[1]
    rows = up_buf.shape[1]
    main = (rows - MIDDLE) // 2
    half = main // 2
    own_rows = main + MIDDLE
    t_core = t + 1 - 2 * c
    t_x = t + 2 - 4 * x
    t_xcore = t_core + 2 - 4 * x
    f_y = f + 1 - 2 * y
    is_end = (z == 0) | (z == deep - 1)

    def cols(tp):
        return pl.ds(pl.multiple_of(tp * width, width), width)

    def seq(i):
        p, q = i // 2, i % 2
        flip = z // 2
        near = z + flip * (deep - 1 - 2 * z)
        v = deep - 1 - p + near * (p // 2) * (2 * p - 5)
        return 2 * (v + flip * (deep - 1 - 2 * v)) + (1 - q) * (1 - y) + q * y

    def remote(src, dst, send, recv, fs, tp):
        return pltpu.make_async_remote_copy(
            src_ref=src, dst_ref=dst, send_sem=send, recv_sem=recv,
            device_id=(fs, tp), device_id_type=MESH,
        )

    lower = pl.ds(pl.multiple_of((main + MIDDLE) * x, 8), main)
    other = pl.ds(pl.multiple_of((main + MIDDLE) * (1 - x), 8), main)
    middle = pl.ds(main, MIDDLE)
    first, second, last = pl.ds(0, main), pl.ds(main, main), pl.ds(2 * main, MIDDLE)

    plan = [
        (down_hbm.at[other], swap_buf.at[first]),
        (down_hbm.at[middle], swap_buf.at[middle]),
        (down_hbm.at[lower], down_buf.at[f, first, cols(t)]),
        (down_hbm.at[middle], down_buf.at[f, middle, cols(t)]),
        (cot_hbm, cot_buf.at[:, cols(t)]),
        (up_hbm.at[lower], up_buf.at[f, first]),
        (up_hbm.at[other], up_buf.at[f, second]),
        (up_hbm.at[middle], up_buf.at[f, last]),
        (in_hbm, in_buf),
        (pre_hbm.at[:, lower], pre_buf.at[:, first]),
        (pre_hbm.at[:, middle], pre_buf.at[:, middle]),
    ]
    local = [
        pltpu.make_async_copy(src, dst, local_sem.at[k]) for k, (src, dst) in enumerate(plan)
    ]
    for copy in local:
        copy.start()

    def swap_copy():
        return remote(
            swap_buf, down_buf.at[f, :, cols(t)], swap_send.at[0], down_recv.at[f, t], f, t_x
        )

    def cot_copy(src_t, slot, tp):
        block = cot_buf.at[:, cols(src_t)]
        return remote(block, block, cot_send.at[slot], cot_recv.at[src_t], f, tp)

    def piece(k):
        return t if k == 0 else t_x

    def down_copy(src_f, k, send, fs, tp):
        block = down_buf.at[src_f, :, cols(piece(k))]
        return remote(block, block, send, down_recv.at[src_f, piece(k)], fs, tp)

    def down_z(src_f, k, step):
        return down_copy(src_f, k, dz_send.at[(1 + step) // 2, src_f // 2, k], f + 2 * step, t)

    def down_y(src_f, k):
        return down_copy(src_f, k, dy_send.at[src_f // 2, k], f_y, t)

    def down_c(src_f, k):
        return down_copy(src_f, k, dc_send.at[src_f, k], f, t_core)

    def up_copy(src_f, send, fs):
        return remote(up_buf.at[src_f], up_buf.at[src_f], send, up_recv.at[src_f], fs, t)

    def up_z(src_f, step):
        return up_copy(src_f, uz_send.at[(1 + step) // 2, src_f // 2], f + 2 * step)

    def up_y(src_f):
        return up_copy(src_f, uy_send.at[src_f // 2], f_y)

    def grad_x(src_f):
        src = grad.at[src_f, pl.ds(pl.multiple_of(half * c, half), half)]
        dst = grad.at[src_f, pl.ds(pl.multiple_of(main + half * c, half), half)]
        return remote(src, dst, gx_send.at[src_f], gx_recv.at[src_f], f, t_x)

    def grad_c(src_f):
        block = grad.at[src_f, pl.ds(pl.multiple_of(main + half * c, half), half)]
        return remote(block, block, gc_send.at[src_f], gc_recv.at[src_f], f, t_core)

    parts = (pl.ds(0, main), pl.ds(main, own_rows))

    def sum_copy(src_f, part, step):
        return remote(
            out_buf.at[src_f, parts[part]], in_sum.at[(1 - step) // 2, src_f, parts[part]],
            rs_send.at[src_f, part], rs_recv.at[(1 - step) // 2, src_f, part], f + 2 * step, t,
        )

    def y_copy(part):
        return remote(
            out_buf.at[f_y, parts[part]], y_in.at[parts[part]],
            rs_send.at[f_y, part], y_recv.at[part], f_y, t,
        )

    def inside(zz):
        return (zz >= 0) & (zz < deep)

    barrier = pltpu.get_barrier_semaphore()
    for peer in ((f_y, t), (f, t_core), (f, t_x)):
        pl.semaphore_signal(barrier, inc=1, device_id=peer, device_id_type=MESH)
    for step in (-1, 1):
        @pl.when(inside(z + step))
        def _():
            pl.semaphore_signal(barrier, inc=1, device_id=(f + 2 * step, t), device_id_type=MESH)
    for k in range(5):
        local[k].wait()
    pl.semaphore_wait(barrier, 5 - is_end.astype(jnp.int32))

    def forward_down(src_f, k, steps, act):
        for step in steps:
            @pl.when(inside(z + step))
            def _():
                act(down_z(src_f, k, step))
        act(down_y(src_f, k))
        act(down_c(src_f, k))

    def start(copy):
        copy.start()

    def finish(copy):
        copy.wait_send()

    def arrived_down(src_f, tp):
        block = down_buf.at[src_f, :, cols(tp)]
        remote(block, block, swap_send.at[0], down_recv.at[src_f, tp], f, t_core).wait_recv()

    def arrived_cot(src_t):
        cot_copy(src_t, 0, t_core).wait_recv()

    def line(d, k):
        for sign in (-1, 1):
            @pl.when(inside(z + sign * d))
            def _():
                src = f + 2 * sign * d
                arrived_down(src, piece(k))
                forward_down(src, k, (-sign,), start)

    def beside(d, k):
        for sign in (-1, 1) if d else (1,):
            @pl.when(inside(z + sign * d))
            def _():
                src = f_y + 2 * sign * d
                arrived_down(src, piece(k))
                down_c(src, k).start()

    def turn(tp):
        cot_turned[cols(tp)] = cot_buf[:, cols(tp)].T

    swap_copy().start()
    forward_down(f, 0, (-1, 1), start)
    cot_copy(t, 1, t_x).start()
    cot_copy(t, 0, t_core).start()
    turn(t)
    arrived_down(f, t_x)
    forward_down(f, 1, (-1, 1), start)
    line(1, 0)
    beside(0, 0)
    for k in range(5, len(local)):
        local[k].wait()
    arrived_cot(t_core)
    turn(t_core)
    line(1, 1)
    for step in (-1, 1):
        @pl.when(inside(z + step) & (z // 2 == (1 - step) // 2))
        def _():
            up_z(f, step).start()
    beside(0, 1)
    line(2, 0)
    beside(1, 0)
    line(2, 1)
    beside(1, 1)
    arrived_cot(t_x)
    cot_copy(t_x, 2, t_core).start()
    turn(t_x)
    line(3, 0)
    beside(2, 0)
    line(3, 1)
    for step in (-1, 1):
        @pl.when(inside(z + step) & (z // 2 != (1 - step) // 2))
        def _():
            up_z(f, step).start()
    up_y(f).start()
    beside(2, 1)
    beside(3, 0)
    beside(3, 1)
    arrived_cot(t_xcore)
    turn(t_xcore)

    def relay(src, part):
        area = parts[part]
        zd = src // 2

        @pl.when((zd >= z) & (z > 0))
        def _():
            sum_copy(src, part, 1).wait_recv()
            held[src, area] = held[src, area] + in_sum[0, src, area].astype(jnp.float32)

        @pl.when((zd <= z) & (z < deep - 1))
        def _():
            sum_copy(src, part, -1).wait_recv()
            held[src, area] = held[src, area] + in_sum[1, src, area].astype(jnp.float32)

        @pl.when(src != f)
        def _():
            out_buf[src, area] = held[src, area].astype(jnp.bfloat16)

        @pl.when(zd > z)
        def _():
            sum_copy(src, part, 1).start()

        @pl.when(zd < z)
        def _():
            sum_copy(src, part, -1).start()

        @pl.when(src == f_y)
        def _():
            y_copy(part).start()

    def head(src):
        return is_end & (src // 2 != z)

    def produce(i, carry):
        src = seq(i)
        arrived_down(src, t_core)
        arrived_down(src, t_xcore)
        hidden = jnp.dot(down_buf[src], cot_turned[...], preferred_element_type=jnp.float32)
        grad_pre = (
            2.0 * hidden * jnp.maximum(pre_buf[src].astype(jnp.float32), 0.0)
        ).astype(jnp.bfloat16)
        grad[src, first] = grad_pre[:main]
        grad[src, last] = grad_pre[main:]
        grad_x(src).start()
        held[src, first] = jnp.dot(
            grad_pre[:main], in_buf[...], preferred_element_type=jnp.float32
        )

        @pl.when(head(src))
        def _():
            relay(src, 0)

        return carry

    lax.fori_loop(0, n, produce, 0)

    def step(i, carry):
        @pl.when(i < n)
        def _():
            src = seq(i)
            grad_x(src).wait_recv()
            grad_c(src).start()

        for d in range(1, deep):
            for sign in (-1, 1):
                @pl.when((i == 2 * (d - 1)) & inside(z + sign * d))
                def _():
                    src = f + 2 * sign * d
                    up_y(src).wait_recv()
                    up_y(src).start()

                    @pl.when(inside(z - sign))
                    def _():
                        up_z(src, -sign).start()

        @pl.when((i > 0) & (i <= n))
        def _():
            src = seq(i - 1)
            grad_c(src).wait_recv()
            held[src, parts[1]] = jnp.dot(
                grad[src, parts[1]], in_buf[...], preferred_element_type=jnp.float32
            )

            @pl.when(head(src))
            def _():
                relay(src, 1)

        @pl.when(i < n)
        def _():
            src = seq(i)

            @pl.when(jnp.logical_not(head(src)))
            def _():
                relay(src, 0)

        @pl.when(i >= LAG)
        def _():
            src = seq(i - LAG)

            @pl.when(jnp.logical_not(head(src)))
            def _():
                relay(src, 1)

        return carry

    lax.fori_loop(0, n + LAG - 1, step, 0)

    for k in range(deep):
        up_y(2 * k + 1 - y).wait_recv()
    gi = jnp.zeros(gi_ref.shape, jnp.float32)
    for block in range(n):
        gi = gi + lax.dot_general(
            grad[block], up_buf[block], (((0,), (0,)), ((), ())),
            preferred_element_type=jnp.float32,
        )
    gi_ref[...] = gi.astype(gi_ref.dtype)
    relay(f, 1)

    root = jnp.sqrt(jnp.float32(token_total))
    y_copy(0).wait_recv()
    gu_ref[lower] = (held[f, first] + y_in[first].astype(jnp.float32)) / root
    y_copy(1).wait_recv()
    gu_ref[other] = (held[f, second] + y_in[second].astype(jnp.float32)) / root
    gu_ref[middle] = (held[f, last] + y_in[last].astype(jnp.float32)) / root

    swap_copy().wait_send()
    for slot, (src_t, tp) in enumerate(((t, t_core), (t, t_x), (t_x, t_core))):
        cot_copy(src_t, slot, tp).wait_send()
    for k in range(2):
        forward_down(f, k, (-1, 1), finish)
        down_c(f_y, k).wait_send()
    for step_ in (-1, 1):
        @pl.when(inside(z + step_))
        def _():
            up_z(f, step_).wait_send()
    up_y(f).wait_send()
    for d in range(1, deep):
        for sign in (-1, 1):
            @pl.when(inside(z + sign * d))
            def _():
                src = f + 2 * sign * d
                for k in range(2):
                    forward_down(src, k, (-sign,), finish)
                    down_c(f_y + 2 * sign * d, k).wait_send()
                up_y(src).wait_send()

                @pl.when(inside(z - sign))
                def _():
                    up_z(src, -sign).wait_send()

    def drain(src, carry):
        grad_x(src).wait_send()
        grad_c(src).wait_send()
        for part in range(2):
            @pl.when(src // 2 > z)
            def _():
                sum_copy(src, part, 1).wait_send()

            @pl.when(src // 2 < z)
            def _():
                sum_copy(src, part, -1).wait_send()

        return carry

    lax.fori_loop(0, n, drain, 0)
    for part in range(2):
        y_copy(part).wait_send()


def settle(gi_ref, gu_ref, gi_out, gu_out):
    gi_out[...] = gi_ref[...]
    gu_out[...] = gu_ref[...]


def fused(n, tp, cotangent, inputs, pre_act, w_up, w_down):
    tokens, width = cotangent.shape
    rows = w_down.shape[0]
    own_rows = (rows - MIDDLE) // 2 + MIDDLE
    deep = n // 2
    dma = pltpu.SemaphoreType.DMA
    vmem = pl.BlockSpec(memory_space=pltpu.VMEM)
    anywhere = pl.BlockSpec(memory_space=pl.ANY)
    shapes = (
        jax.ShapeDtypeStruct((tokens, width), jnp.bfloat16),
        jax.ShapeDtypeStruct((rows, width), jnp.float32),
    )
    results = pl.pallas_call(
        functools.partial(kernel, n, tokens * n),
        out_shape=shapes,
        in_specs=[anywhere] * 5,
        out_specs=(vmem, vmem),
        scratch_shapes=[
            pltpu.VMEM((tokens, tp * width), jnp.bfloat16),
            pltpu.VMEM((tp * width, tokens), jnp.bfloat16),
            pltpu.VMEM((tokens, width), jnp.bfloat16),
            pltpu.VMEM((n, own_rows, tp * width), jnp.bfloat16),
            pltpu.VMEM((own_rows, width), jnp.bfloat16),
            pltpu.VMEM((n, rows, width), jnp.bfloat16),
            pltpu.VMEM((n, own_rows, tokens), jnp.bfloat16),
            pltpu.VMEM((n, rows, tokens), jnp.bfloat16),
            pltpu.VMEM((n, rows, width), jnp.float32),
            pltpu.VMEM((n, rows, width), jnp.bfloat16),
            pltpu.VMEM((2, n, rows, width), jnp.bfloat16),
            pltpu.VMEM((rows, width), jnp.bfloat16),
            dma((11,)),
            dma((3,)), dma((tp,)), dma((1,)),
            dma((2, deep, 2)), dma((deep, 2)), dma((n, 2)), dma((n, tp)),
            dma((2, deep)), dma((deep,)), dma((n,)),
            dma((n,)), dma((n,)), dma((n,)), dma((n,)),
            dma((n, 2)), dma((2, n, 2)), dma((2,)),
        ],
        compiler_params=pltpu.CompilerParams(
            collective_id=0, has_side_effects=True, vmem_limit_bytes=60 * 2**20
        ),
    )(cotangent, inputs, pre_act.T.reshape(n, rows, tokens), w_up, w_down)
    return pl.pallas_call(
        settle, out_shape=shapes, in_specs=[vmem, vmem], out_specs=(vmem, vmem)
    )(*results)


def gathered(cotangent, inputs, pre_act, w_up, w_down):
    token_total = cotangent.shape[0] * lax.axis_size("fs")
    full_cotangent = lax.all_gather(cotangent, "tp", axis=1, tiled=True)
    down_whole = lax.all_gather(w_down, "tp", axis=1, tiled=True)
    grad_hidden = times_rows(full_cotangent, lax.all_gather(down_whole, "fs", axis=0, tiled=True))
    grad_pre = (2.0 * grad_hidden * jnp.maximum(pre_act.astype(jnp.float32), 0.0)).astype(
        jnp.bfloat16
    )
    grad_input = jnp.dot(
        grad_pre, lax.all_gather(w_up, "fs", axis=0, tiled=True), preferred_element_type=jnp.float32
    )
    grad_share = lax.psum_scatter(
        lax.dot_general(
            grad_pre, inputs, (((0,), (0,)), ((), ())), preferred_element_type=jnp.float32
        ),
        "fs",
        scatter_dimension=0,
        tiled=True,
    )
    grad_up = grad_share / jnp.sqrt(jnp.float32(token_total))
    return (grad_input.astype(jnp.bfloat16), grad_up)


def solution(mesh):
    n, tp = mesh.shape["fs"], mesh.shape["tp"]

    def local(cotangent, inputs, pre_act, w_up, w_down):
        rows, width = w_down.shape
        fits = tp == 4 and n == 8 and rows % 128 == MIDDLE and width % 128 == 0
        if fits:
            return fused(n, tp, cotangent, inputs, pre_act, w_up, w_down)
        return gathered(cotangent, inputs, pre_act, w_up, w_down)

    return jax.shard_map(
        local,
        mesh=mesh,
        in_specs=(P("fs", "tp"), P("fs", "tp"), P("fs", None), P("fs", "tp"), P("fs", "tp")),
        out_specs=(P("fs", "tp"), P("fs", "tp")),
        check_vma=False,
    )
```

```python
import functools

import jax
import jax.numpy as jnp
from jax import lax
from jax.experimental import pallas as pl
from jax.experimental.pallas import tpu as pltpu
from jax.sharding import PartitionSpec as P

MESH = pl.DeviceIdType.MESH
MIDDLE = 8
PU = (0, 1, 4)


def times_rows(left, piece):
    return lax.dot_general(
        left, piece, (((1,), (1,)), ((), ())), preferred_element_type=jnp.float32
    )


def toggled(index, mask, bits):
    for bit in range(bits):
        unit = 2**bit
        index = index + unit * ((mask // unit) % 2) * (1 - 2 * ((index // unit) % 2))
    return index


def kernel(
    n, token_total,
    cot_hbm, in_hbm, pre_hbm, up_hbm, down_hbm,
    gi_ref, gu_ref,
    cot_buf, cot_turned, in_buf, down_buf, swap_buf, up_buf, pre_buf, grad, held,
    y_out, y_in, z_out, z_in,
    local_sem, cot_send, cot_recv, swap_send, dz_send, dy_send, dc_send, down_recv,
    uz_send, uy_send, up_recv, rest_send, rest_recv, gx_send, gx_recv, gc_send, gc_recv,
    ys_send, ys_recv, zs_send, zs_recv,
):
    deep = n // 2
    bits = n.bit_length() - 1
    f = lax.axis_index("fs")
    t = lax.axis_index("tp")
    z, y = f // 2, f % 2
    x, c = t // 2, t % 2
    width = in_buf.shape[1]
    rows = up_buf.shape[1]
    main = (rows - MIDDLE) // 2
    half = main // 2
    own_rows = main + MIDDLE
    t_core = t + 1 - 2 * c
    t_x = t + 2 - 4 * x
    t_xcore = t_core + 2 - 4 * x
    f_y = f + 1 - 2 * y
    is_mid = (z > 0) & (z < deep - 1)

    def cols(tp):
        return pl.ds(pl.multiple_of(tp * width, width), width)

    def far(m):
        return toggled(f, 2 * m, bits)

    def seq(i):
        pair = i // 2
        return toggled(f, 2 * ((pair + 1) % deep) + (i + 1) % 2, bits)

    def remote(src, dst, send, recv, fs, tp):
        return pltpu.make_async_remote_copy(
            src_ref=src, dst_ref=dst, send_sem=send, recv_sem=recv,
            device_id=(fs, tp), device_id_type=MESH,
        )

    lower = pl.ds(pl.multiple_of((main + MIDDLE) * x, 8), main)
    other = pl.ds(pl.multiple_of((main + MIDDLE) * (1 - x), 8), main)
    middle = pl.ds(main, MIDDLE)
    first, second, last = pl.ds(0, main), pl.ds(main, main), pl.ds(2 * main, MIDDLE)
    parts = (first, pl.ds(main, own_rows))

    plan = [
        (down_hbm.at[other], swap_buf.at[first]),
        (down_hbm.at[middle], swap_buf.at[middle]),
        (down_hbm.at[lower], down_buf.at[f, first, cols(t)]),
        (down_hbm.at[middle], down_buf.at[f, middle, cols(t)]),
        (cot_hbm, cot_buf.at[:, cols(t)]),
        (up_hbm.at[lower], up_buf.at[f, first]),
        (up_hbm.at[other], up_buf.at[f, second]),
        (up_hbm.at[middle], up_buf.at[f, last]),
        (in_hbm, in_buf),
        (pre_hbm.at[:, lower], pre_buf.at[:, first]),
        (pre_hbm.at[:, middle], pre_buf.at[:, middle]),
    ]
    local = [
        pltpu.make_async_copy(src, dst, local_sem.at[k]) for k, (src, dst) in enumerate(plan)
    ]
    for copy in local:
        copy.start()

    def swap_copy():
        return remote(
            swap_buf, down_buf.at[f, :, cols(t)], swap_send.at[0], down_recv.at[f, t], f, t_x
        )

    def cot_copy(src_t, slot, tp):
        block = cot_buf.at[:, cols(src_t)]
        return remote(block, block, cot_send.at[slot], cot_recv.at[src_t], f, tp)

    def piece(k):
        return t if k == 0 else t_x

    def down_copy(src_f, k, send, fs, tp):
        block = down_buf.at[src_f, :, cols(piece(k))]
        return remote(block, block, send, down_recv.at[src_f, piece(k)], fs, tp)

    def down_z(src_f, k, step):
        return down_copy(src_f, k, dz_send.at[(1 + step) // 2, src_f // 2, k], f + 2 * step, t)

    def down_y(src_f, k):
        return down_copy(src_f, k, dy_send.at[src_f // 2, k], f_y, t)

    def down_c(src_f, k):
        return down_copy(src_f, k, dc_send.at[src_f, k], f, t_core)

    def up_copy(src_f, area, send, recv, fs):
        block = up_buf.at[src_f, area]
        return remote(block, block, send, recv.at[src_f], fs, t)

    def up_z(m):
        return up_copy(f, pl.ds(0, rows), uz_send.at[m], up_recv, far(m))

    def rest_z(m):
        return up_copy(f_y, parts[1], rest_send.at[m], rest_recv, far(m))

    def up_y(src_f):
        return up_copy(src_f, parts[0], uy_send.at[src_f // 2], up_recv, f_y)

    def rest_y():
        return up_copy(f, parts[1], uy_send.at[deep], rest_recv, f_y)

    def grad_x(src_f):
        src = grad.at[src_f, pl.ds(pl.multiple_of(half * c, half), half)]
        dst = grad.at[src_f, pl.ds(pl.multiple_of(main + half * c, half), half)]
        return remote(src, dst, gx_send.at[src_f], gx_recv.at[src_f], f, t_x)

    def grad_c(src_f):
        block = grad.at[src_f, pl.ds(pl.multiple_of(main + half * c, half), half)]
        return remote(block, block, gc_send.at[src_f], gc_recv.at[src_f], f, t_core)

    def y_copy(pair, part):
        return remote(
            y_out.at[pair, parts[part]], y_in.at[pair, parts[part]],
            ys_send.at[pair, part], ys_recv.at[pair, part], f_y, t,
        )

    def z_copy(pair, part):
        return remote(
            z_out.at[pair, parts[part]], z_in.at[pair, parts[part]],
            zs_send.at[pair, part], zs_recv.at[pair, part], far(pair + 1), t,
        )

    def inside(zz):
        return (zz >= 0) & (zz < deep)

    barrier = pltpu.get_barrier_semaphore()
    peers = [(far(m), t) for m in range(1, deep)] + [(f_y, t), (f, t_core), (f, t_x)]
    for peer in peers:
        pl.semaphore_signal(barrier, inc=1, device_id=peer, device_id_type=MESH)
    for k in range(8):
        local[k].wait()
    pl.semaphore_wait(barrier, len(peers))

    def arrived_down(src_f, tp):
        block = down_buf.at[src_f, :, cols(tp)]
        remote(block, block, swap_send.at[0], down_recv.at[src_f, tp], f, t_core).wait_recv()

    def arrived_cot(src_t):
        cot_copy(src_t, 0, t_core).wait_recv()

    def forward_down(src_f, k, steps, act):
        for step in steps:
            @pl.when(inside(z + step))
            def _():
                act(down_z(src_f, k, step))
        act(down_y(src_f, k))
        act(down_c(src_f, k))

    def start(copy):
        copy.start()

    def finish(copy):
        copy.wait_send()

    def line(d, k):
        for sign in (-1, 1):
            @pl.when(inside(z + sign * d))
            def _():
                src = f + 2 * sign * d
                arrived_down(src, piece(k))
                forward_down(src, k, (-sign,), start)

    def beside(d, k):
        for sign in (-1, 1) if d else (1,):
            @pl.when(inside(z + sign * d))
            def _():
                src = f_y + 2 * sign * d
                arrived_down(src, piece(k))
                down_c(src, k).start()

    def offer_up():
        up_z(2).start()
        up_z(1).start()

        @pl.when(is_mid)
        def _():
            up_z(3).start()

        up_copy(f_y, parts[1], uy_send.at[deep], rest_recv, f_y).wait_recv()
        rest_z(2).start()
        rest_z(1).start()

        @pl.when(is_mid)
        def _():
            rest_z(3).start()

    def turn(tp):
        cot_turned[cols(tp)] = cot_buf[:, cols(tp)].T

    swap_copy().start()
    forward_down(f, 0, (-1, 1), start)
    rest_y().start()
    cot_copy(t, 1, t_x).start()
    cot_copy(t, 0, t_core).start()
    turn(t)
    arrived_down(f, t_x)
    forward_down(f, 1, (-1, 1), start)
    line(1, 0)
    beside(0, 0)
    for k in range(8, len(local)):
        local[k].wait()
    arrived_cot(t_core)
    turn(t_core)
    line(1, 1)
    beside(0, 1)
    line(2, 0)
    beside(1, 0)
    line(2, 1)
    offer_up()
    line(3, 0)
    beside(1, 1)
    beside(2, 0)
    arrived_cot(t_x)
    cot_copy(t_x, 2, t_core).start()
    turn(t_x)
    arrived_cot(t_xcore)
    turn(t_xcore)

    def share(pair, part, across, value):
        if across:
            y_out[pair, parts[part]] = value.astype(jnp.bfloat16)
            y_copy(pair, part).start()
        else:
            held[pair, parts[part]] = value

    def combine(pair, part):
        y_copy(pair, part).wait_recv()
        area = parts[part]
        z_out[pair, area] = (
            held[pair, area] + y_in[pair, area].astype(jnp.float32)
        ).astype(jnp.bfloat16)
        z_copy(pair, part).start()

    def produce(pair):
        for across in (1, 0):
            src = seq(2 * pair + 1 - across)
            arrived_down(src, t_core)
            arrived_down(src, t_xcore)
            hidden = jnp.dot(down_buf[src], cot_turned[...], preferred_element_type=jnp.float32)
            grad_pre = (
                2.0 * hidden * jnp.maximum(pre_buf[src].astype(jnp.float32), 0.0)
            ).astype(jnp.bfloat16)
            grad[src, first] = grad_pre[:main]
            grad[src, last] = grad_pre[main:]
            grad_x(src).start()
            share(pair, 0, across, jnp.dot(
                grad_pre[:main], in_buf[...], preferred_element_type=jnp.float32
            ))

    def produce_step(pair, carry):
        @pl.when(pair == 1)
        def _():
            line(3, 1)
            beside(2, 1)
            beside(3, 0)
            up_y(f).start()

        @pl.when(pair == 2)
        def _():
            beside(3, 1)

        produce(pair)
        return carry

    lax.fori_loop(0, deep, produce_step, 0)

    def relays():
        return (
            up_copy(far(2), pl.ds(0, rows), uz_send.at[0], up_recv, far(1)),
            up_copy(toggled(f, 5, bits), parts[1], rest_send.at[0], rest_recv, far(1)),
        )

    def pass_up(m):
        up_copy(far(m), pl.ds(0, rows), uz_send.at[m], up_recv, f_y).wait_recv()
        if m == 2:
            @pl.when(is_mid)
            def _():
                whole, rest = relays()
                whole.start()
                rest.wait_recv()
                rest.start()

        up_y(far(m)).start()

    def step(i, carry):
        @pl.when(i < n)
        def _():
            src = seq(i)
            grad_x(src).wait_recv()
            grad_c(src).start()

        @pl.when((i > 0) & (i <= n))
        def _():
            j = i - 1
            src = seq(j)
            pair = j // 2
            grad_c(src).wait_recv()
            part = jnp.dot(
                grad[src, parts[1]], in_buf[...], preferred_element_type=jnp.float32
            )

            @pl.when(j % 2 == 0)
            def _():
                share(pair, 1, 1, part)

            @pl.when(j % 2 == 1)
            def _():
                share(pair, 1, 0, part)

        @pl.when(i < deep - 1)
        def _():
            combine(i, 0)

        @pl.when((i % 2 == 1) & (i >= 3) & (i < 2 * deep))
        def _():
            combine((i - 3) // 2, 1)

        for k, m in ((PU[0], 2), (PU[1], 1), (PU[2], 3)):
            @pl.when(i == k)
            def _():
                pass_up(m)

        return carry

    lax.fori_loop(0, n + 1, step, 0)

    for m in range(deep):
        src = toggled(f, 2 * m + 1, bits)
        up_y(src).wait_recv()
        rest = up_copy(src, parts[1], uy_send.at[deep], rest_recv, f_y)
        if m == 2:
            @pl.when(jnp.logical_not(is_mid))
            def _():
                rest.wait_recv()
        elif m:
            rest.wait_recv()
    gi = jnp.zeros(gi_ref.shape, jnp.float32)
    for block in range(n):
        gi = gi + lax.dot_general(
            grad[block], up_buf[block], (((0,), (0,)), ((), ())),
            preferred_element_type=jnp.float32,
        )
    gi_ref[...] = gi.astype(gi_ref.dtype)

    root = jnp.sqrt(jnp.float32(token_total))
    for part, area in enumerate(parts):
        total = held[deep - 1, area]
        for pair in range(deep - 1):
            z_copy(pair, part).wait_recv()
            total = total + z_in[pair, area].astype(jnp.float32)
        y_copy(deep - 1, part).wait_recv()
        total = (total + y_in[deep - 1, area].astype(jnp.float32)) / root
        if part == 0:
            gu_ref[lower] = total
        else:
            gu_ref[other] = total[:main]
            gu_ref[middle] = total[main:]

    swap_copy().wait_send()
    rest_y().wait_send()
    for slot, (src_t, tp) in enumerate(((t, t_core), (t, t_x), (t_x, t_core))):
        cot_copy(src_t, slot, tp).wait_send()
    for k in range(2):
        forward_down(f, k, (-1, 1), finish)
        down_c(f_y, k).wait_send()
    for m in range(1, deep):
        if m < 3:
            up_z(m).wait_send()
            rest_z(m).wait_send()
        up_y(far(m)).wait_send()

    @pl.when(is_mid)
    def _():
        up_z(3).wait_send()
        rest_z(3).wait_send()
        for copy in relays():
            copy.wait_send()

    up_y(f).wait_send()
    for d in range(1, deep):
        for sign in (-1, 1):
            @pl.when(inside(z + sign * d))
            def _():
                src = f + 2 * sign * d
                for k in range(2):
                    forward_down(src, k, (-sign,), finish)
                    down_c(f_y + 2 * sign * d, k).wait_send()

    def drain(src, carry):
        grad_x(src).wait_send()
        grad_c(src).wait_send()
        return carry

    lax.fori_loop(0, n, drain, 0)
    for part in range(2):
        for pair in range(deep):
            y_copy(pair, part).wait_send()
            if pair < deep - 1:
                z_copy(pair, part).wait_send()


def settle(gi_ref, gu_ref, gi_out, gu_out):
    gi_out[...] = gi_ref[...]
    gu_out[...] = gu_ref[...]


def fused(n, tp, cotangent, inputs, pre_act, w_up, w_down):
    tokens, width = cotangent.shape
    rows = w_down.shape[0]
    own_rows = (rows - MIDDLE) // 2 + MIDDLE
    deep = n // 2
    dma = pltpu.SemaphoreType.DMA
    vmem = pl.BlockSpec(memory_space=pltpu.VMEM)
    anywhere = pl.BlockSpec(memory_space=pl.ANY)
    shapes = (
        jax.ShapeDtypeStruct((tokens, width), jnp.bfloat16),
        jax.ShapeDtypeStruct((rows, width), jnp.float32),
    )
    results = pl.pallas_call(
        functools.partial(kernel, n, tokens * n),
        out_shape=shapes,
        in_specs=[anywhere] * 5,
        out_specs=(vmem, vmem),
        scratch_shapes=[
            pltpu.VMEM((tokens, tp * width), jnp.bfloat16),
            pltpu.VMEM((tp * width, tokens), jnp.bfloat16),
            pltpu.VMEM((tokens, width), jnp.bfloat16),
            pltpu.VMEM((n, own_rows, tp * width), jnp.bfloat16),
            pltpu.VMEM((own_rows, width), jnp.bfloat16),
            pltpu.VMEM((n, rows, width), jnp.bfloat16),
            pltpu.VMEM((n, own_rows, tokens), jnp.bfloat16),
            pltpu.VMEM((n, rows, tokens), jnp.bfloat16),
            pltpu.VMEM((deep, rows, width), jnp.float32),
            pltpu.VMEM((deep, rows, width), jnp.bfloat16),
            pltpu.VMEM((deep, rows, width), jnp.bfloat16),
            pltpu.VMEM((deep - 1, rows, width), jnp.bfloat16),
            pltpu.VMEM((deep - 1, rows, width), jnp.bfloat16),
            dma((11,)),
            dma((3,)), dma((tp,)), dma((1,)),
            dma((2, deep, 2)), dma((deep, 2)), dma((n, 2)), dma((n, tp)),
            dma((deep,)), dma((deep + 1,)), dma((n,)), dma((deep,)), dma((n,)),
            dma((n,)), dma((n,)), dma((n,)), dma((n,)),
            dma((deep, 2)), dma((deep, 2)), dma((deep - 1, 2)), dma((deep - 1, 2)),
        ],
        compiler_params=pltpu.CompilerParams(
            collective_id=0, has_side_effects=True, vmem_limit_bytes=60 * 2**20
        ),
    )(cotangent, inputs, pre_act.T.reshape(n, rows, tokens), w_up, w_down)
    return pl.pallas_call(
        settle, out_shape=shapes, in_specs=[vmem, vmem], out_specs=(vmem, vmem)
    )(*results)


def gathered(cotangent, inputs, pre_act, w_up, w_down):
    token_total = cotangent.shape[0] * lax.axis_size("fs")
    full_cotangent = lax.all_gather(cotangent, "tp", axis=1, tiled=True)
    down_whole = lax.all_gather(w_down, "tp", axis=1, tiled=True)
    grad_hidden = times_rows(full_cotangent, lax.all_gather(down_whole, "fs", axis=0, tiled=True))
    grad_pre = (2.0 * grad_hidden * jnp.maximum(pre_act.astype(jnp.float32), 0.0)).astype(
        jnp.bfloat16
    )
    grad_input = jnp.dot(
        grad_pre, lax.all_gather(w_up, "fs", axis=0, tiled=True), preferred_element_type=jnp.float32
    )
    grad_share = lax.psum_scatter(
        lax.dot_general(
            grad_pre, inputs, (((0,), (0,)), ((), ())), preferred_element_type=jnp.float32
        ),
        "fs",
        scatter_dimension=0,
        tiled=True,
    )
    grad_up = grad_share / jnp.sqrt(jnp.float32(token_total))
    return (grad_input.astype(jnp.bfloat16), grad_up)


def solution(mesh):
    n, tp = mesh.shape["fs"], mesh.shape["tp"]

    def local(cotangent, inputs, pre_act, w_up, w_down):
        rows, width = w_down.shape
        fits = tp == 4 and n == 8 and rows % 128 == MIDDLE and width % 128 == 0
        if fits:
            return fused(n, tp, cotangent, inputs, pre_act, w_up, w_down)
        return gathered(cotangent, inputs, pre_act, w_up, w_down)

    return jax.shard_map(
        local,
        mesh=mesh,
        in_specs=(P("fs", "tp"), P("fs", "tp"), P("fs", None), P("fs", "tp"), P("fs", "tp")),
        out_specs=(P("fs", "tp"), P("fs", "tp")),
        check_vma=False,
    )
```

```python
import functools

import jax
import jax.numpy as jnp
from jax import lax
from jax.experimental import pallas as pl
from jax.experimental.pallas import tpu as pltpu
from jax.sharding import PartitionSpec as P

MESH = pl.DeviceIdType.MESH
MIDDLE = 8
ORDER = (
    ("uz", 1), ("rest",), ("cots",), ("line", 1, 0), ("core",), ("own",), ("rz", 3),
    ("line", 3, 0), ("line", 2, 0), ("line", 1, 1), ("uz", 3), ("rz", 2), ("cot",),
    ("line", 3, 1), ("uz", 2), ("line", 2, 1), ("beside", 0, 1), ("both",), ("beside", 0, 0),
    ("beside", 2, 0), ("make", 1), ("make", 6), ("beside", 1, 1), ("beside", 1, 0), ("make", 0),
    ("beside", 3, 0), ("beside", 3, 1), ("make", 4), ("beside", 2, 1), ("ufy", 1), ("rz", 1),
    ("make", 2), ("make", 3), ("make", 5), ("comb", 0, 0), ("gx", 1), ("comb", 2, 0), ("gx", 6),
    ("up",), ("gx", 0), ("make", 7), ("gx", 4), ("rrel",), ("more", 0), ("comb", 1, 0),
    ("gx", 2), ("more", 4), ("gx", 3), ("more", 1), ("more", 2), ("ufy", 2), ("more", 3),
    ("urel",), ("comb", 0, 1), ("gx", 5), ("ufy", 3), ("more", 5), ("comb", 2, 1), ("gx", 7),
    ("comb", 1, 1), ("more", 6), ("more", 7),
)


def times_rows(left, piece):
    return lax.dot_general(
        left, piece, (((1,), (1,)), ((), ())), preferred_element_type=jnp.float32
    )


def toggled(index, mask, bits):
    for bit in range(bits):
        unit = 2**bit
        index = index + unit * ((mask // unit) % 2) * (1 - 2 * ((index // unit) % 2))
    return index


def kernel(
    n, token_total,
    cot_hbm, in_hbm, pre_hbm, up_hbm, down_hbm,
    gi_ref, gu_ref,
    cot_buf, cot_turned, in_buf, down_buf, swap_buf, up_buf, pre_buf, grad, held,
    y_out, y_in, z_out, z_in,
    local_sem, cot_send, cot_recv, swap_send, dz_send, dy_send, dc_send, down_recv,
    uz_send, uy_send, up_recv, rest_send, rest_recv, gx_send, gx_recv, gc_send, gc_recv,
    ys_send, ys_recv, zs_send, zs_recv,
):
    deep = n // 2
    bits = n.bit_length() - 1
    f = lax.axis_index("fs")
    t = lax.axis_index("tp")
    z, y = f // 2, f % 2
    x, c = t // 2, t % 2
    width = in_buf.shape[1]
    rows = up_buf.shape[1]
    main = (rows - MIDDLE) // 2
    half = main // 2
    own_rows = main + MIDDLE
    t_core = t + 1 - 2 * c
    t_x = t + 2 - 4 * x
    t_xcore = t_core + 2 - 4 * x
    f_y = f + 1 - 2 * y
    is_mid = (z > 0) & (z < deep - 1)

    def cols(tp):
        return pl.ds(pl.multiple_of(tp * width, width), width)

    def far(m):
        return toggled(f, 2 * m, bits)

    def seq(i):
        pair = i // 2
        return toggled(f, 2 * ((pair + 1) % deep) + (i + 1) % 2, bits)

    def remote(src, dst, send, recv, fs, tp):
        return pltpu.make_async_remote_copy(
            src_ref=src, dst_ref=dst, send_sem=send, recv_sem=recv,
            device_id=(fs, tp), device_id_type=MESH,
        )

    lower = pl.ds(pl.multiple_of((main + MIDDLE) * x, 8), main)
    other = pl.ds(pl.multiple_of((main + MIDDLE) * (1 - x), 8), main)
    middle = pl.ds(main, MIDDLE)
    first, second, last = pl.ds(0, main), pl.ds(main, main), pl.ds(2 * main, MIDDLE)
    parts = (first, pl.ds(main, own_rows))

    plan = [
        (down_hbm.at[other], swap_buf.at[first]),
        (down_hbm.at[middle], swap_buf.at[middle]),
        (down_hbm.at[lower], down_buf.at[f, first, cols(t)]),
        (down_hbm.at[middle], down_buf.at[f, middle, cols(t)]),
        (cot_hbm, cot_buf.at[:, cols(t)]),
        (up_hbm.at[lower], up_buf.at[f, first]),
        (up_hbm.at[other], up_buf.at[f, second]),
        (up_hbm.at[middle], up_buf.at[f, last]),
        (in_hbm, in_buf),
        (pre_hbm.at[:, lower], pre_buf.at[:, first]),
        (pre_hbm.at[:, middle], pre_buf.at[:, middle]),
    ]
    local = [
        pltpu.make_async_copy(src, dst, local_sem.at[k]) for k, (src, dst) in enumerate(plan)
    ]
    for copy in local:
        copy.start()

    def swap_copy():
        return remote(
            swap_buf, down_buf.at[f, :, cols(t)], swap_send.at[0], down_recv.at[f, t], f, t_x
        )

    def cot_copy(src_t, slot, tp):
        block = cot_buf.at[:, cols(src_t)]
        return remote(block, block, cot_send.at[slot], cot_recv.at[src_t], f, tp)

    def piece(k):
        return t if k == 0 else t_x

    def down_copy(src_f, k, send, fs, tp):
        block = down_buf.at[src_f, :, cols(piece(k))]
        return remote(block, block, send, down_recv.at[src_f, piece(k)], fs, tp)

    def down_z(src_f, k, step):
        return down_copy(src_f, k, dz_send.at[(1 + step) // 2, src_f // 2, k], f + 2 * step, t)

    def down_y(src_f, k):
        return down_copy(src_f, k, dy_send.at[src_f // 2, k], f_y, t)

    def down_c(src_f, k):
        return down_copy(src_f, k, dc_send.at[src_f, k], f, t_core)

    def up_copy(src_f, area, send, recv, fs):
        block = up_buf.at[src_f, area]
        return remote(block, block, send, recv.at[src_f], fs, t)

    def up_z(m):
        return up_copy(f, pl.ds(0, rows), uz_send.at[m], up_recv, far(m))

    def rest_z(m):
        return up_copy(f_y, parts[1], rest_send.at[m], rest_recv, far(m))

    def up_y(src_f):
        return up_copy(src_f, parts[0], uy_send.at[src_f // 2], up_recv, f_y)

    def rest_y():
        return up_copy(f, parts[1], uy_send.at[deep], rest_recv, f_y)

    def grad_x(src_f):
        src = grad.at[src_f, pl.ds(pl.multiple_of(half * c, half), half)]
        dst = grad.at[src_f, pl.ds(pl.multiple_of(main + half * c, half), half)]
        return remote(src, dst, gx_send.at[src_f], gx_recv.at[src_f], f, t_x)

    def grad_c(src_f):
        block = grad.at[src_f, pl.ds(pl.multiple_of(main + half * c, half), half)]
        return remote(block, block, gc_send.at[src_f], gc_recv.at[src_f], f, t_core)

    def y_copy(pair, part):
        return remote(
            y_out.at[pair, parts[part]], y_in.at[pair, parts[part]],
            ys_send.at[pair, part], ys_recv.at[pair, part], f_y, t,
        )

    def z_copy(pair, part):
        return remote(
            z_out.at[pair, parts[part]], z_in.at[pair, parts[part]],
            zs_send.at[pair, part], zs_recv.at[pair, part], far(pair + 1), t,
        )

    def inside(zz):
        return (zz >= 0) & (zz < deep)

    barrier = pltpu.get_barrier_semaphore()
    for peer in ((f_y, t), (f, t_core), (f, t_x)):
        pl.semaphore_signal(barrier, inc=1, device_id=peer, device_id_type=MESH)
    for step in (-1, 1):
        @pl.when(inside(z + step))
        def _():
            pl.semaphore_signal(barrier, inc=1, device_id=(f + 2 * step, t), device_id_type=MESH)

    for k in range(8):
        local[k].wait()
    pl.semaphore_wait(barrier, 4 + is_mid.astype(jnp.int32))

    def arrived_down(src_f, tp):
        block = down_buf.at[src_f, :, cols(tp)]
        remote(block, block, swap_send.at[0], down_recv.at[src_f, tp], f, t_core).wait_recv()

    def arrived_cot(src_t):
        cot_copy(src_t, 0, t_core).wait_recv()

    def forward_down(src_f, k, steps, act):
        for step in steps:
            @pl.when(inside(z + step))
            def _():
                act(down_z(src_f, k, step))
        act(down_y(src_f, k))
        act(down_c(src_f, k))

    def start(copy):
        copy.start()

    def finish(copy):
        copy.wait_send()

    def arrived_up(src_f):
        up_copy(src_f, pl.ds(0, rows), uz_send.at[0], up_recv, f_y).wait_recv()

    def arrived_rest(src_f):
        up_copy(src_f, parts[1], uy_send.at[deep], rest_recv, f_y).wait_recv()

    def turn(tp):
        cot_turned[cols(tp)] = cot_buf[:, cols(tp)].T

    def share(pair, part, across, value):
        if across:
            y_out[pair, parts[part]] = value.astype(jnp.bfloat16)
            y_copy(pair, part).start()
        else:
            held[pair, parts[part]] = value

    def relay_up():
        return up_copy(far(2), pl.ds(0, rows), uz_send.at[0], up_recv, far(1))

    def relay_rest():
        return up_copy(toggled(f, 5, bits), parts[1], rest_send.at[0], rest_recv, far(1))

    seen = set()

    def once(name, act):
        if name not in seen:
            seen.add(name)
            act()

    def do_own():
        arrived_down(f, t_x)
        forward_down(f, 1, (-1, 1), start)

    def do_line(m, k):
        src = far(m)
        arrived_down(src, piece(k))
        for step in (-1, 1):
            @pl.when(inside(z + step) & ((src < f) == (step > 0)))
            def _():
                down_z(src, k, step).start()

        down_y(src, k).start()
        down_c(src, k).start()

    def do_beside(m, k):
        src = toggled(f, 2 * m + 1, bits)
        arrived_down(src, piece(k))
        down_c(src, k).start()

    def do_cots():
        cot_copy(t, 1, t_x).start()
        cot_copy(t, 0, t_core).start()
        turn(t)

    def do_cot_core():
        arrived_cot(t_core)
        turn(t_core)

    def do_cot_x():
        arrived_cot(t_x)
        cot_copy(t_x, 2, t_core).start()
        turn(t_x)

    def do_cot_xc():
        arrived_cot(t_xcore)
        turn(t_xcore)

    def do_uz(m):
        if m < 3:
            up_z(m).start()
        else:
            @pl.when(is_mid)
            def _():
                up_z(3).start()

    def do_rz(m):
        once("rest", lambda: arrived_rest(f_y))
        if m < 3:
            rest_z(m).start()
        else:
            @pl.when(is_mid)
            def _():
                rest_z(3).start()

    def do_ufy(m):
        once(("up", m), lambda: arrived_up(far(m)))
        up_y(far(m)).start()

    def do_urel():
        once(("up", 2), lambda: arrived_up(far(2)))

        @pl.when(is_mid)
        def _():
            relay_up().start()

    def do_rrel():
        @pl.when(is_mid)
        def _():
            relay_rest().wait_recv()
            relay_rest().start()

    def more_local():
        for k in range(8, len(local)):
            local[k].wait()

    def do_make(i):
        once("local", more_local)
        src = seq(i)
        arrived_down(src, t_core)
        arrived_down(src, t_xcore)
        hidden = jnp.dot(down_buf[src], cot_turned[...], preferred_element_type=jnp.float32)
        grad_pre = (
            2.0 * hidden * jnp.maximum(pre_buf[src].astype(jnp.float32), 0.0)
        ).astype(jnp.bfloat16)
        grad[src, first] = grad_pre[:main]
        grad[src, last] = grad_pre[main:]
        grad_x(src).start()
        share(i // 2, 0, i % 2 == 0, jnp.dot(
            grad_pre[:main], in_buf[...], preferred_element_type=jnp.float32
        ))

    def do_gx(i):
        src = seq(i)
        grad_x(src).wait_recv()
        grad_c(src).start()

    def do_more(i):
        src = seq(i)
        grad_c(src).wait_recv()
        share(i // 2, 1, i % 2 == 0, jnp.dot(
            grad[src, parts[1]], in_buf[...], preferred_element_type=jnp.float32
        ))

    def do_comb(pair, part):
        y_copy(pair, part).wait_recv()
        area = parts[part]
        z_out[pair, area] = (
            held[pair, area] + y_in[pair, area].astype(jnp.float32)
        ).astype(jnp.bfloat16)
        z_copy(pair, part).start()

    swap_copy().start()
    forward_down(f, 0, (-1, 1), start)
    acts = {
        "own": do_own, "line": do_line, "beside": do_beside, "cots": do_cots,
        "core": do_cot_core, "cot": do_cot_x, "both": do_cot_xc,
        "rest": lambda: rest_y().start(), "up": lambda: up_y(f).start(),
        "uz": do_uz, "rz": do_rz, "ufy": do_ufy, "urel": do_urel, "rrel": do_rrel,
        "make": do_make, "gx": do_gx, "more": do_more, "comb": do_comb,
    }
    for name, *values in ORDER:
        acts[name](*values)

    for m in range(deep):
        src = toggled(f, 2 * m + 1, bits)
        up_y(src).wait_recv()
        rest = up_copy(src, parts[1], uy_send.at[deep], rest_recv, f_y)
        if m == 2:
            @pl.when(jnp.logical_not(is_mid))
            def _():
                rest.wait_recv()
        elif m:
            rest.wait_recv()
    gi = jnp.zeros(gi_ref.shape, jnp.float32)
    for block in range(n):
        gi = gi + lax.dot_general(
            grad[block], up_buf[block], (((0,), (0,)), ((), ())),
            preferred_element_type=jnp.float32,
        )
    gi_ref[...] = gi.astype(gi_ref.dtype)

    root = jnp.sqrt(jnp.float32(token_total))
    for part, area in enumerate(parts):
        total = held[deep - 1, area]
        for pair in range(deep - 1):
            z_copy(pair, part).wait_recv()
            total = total + z_in[pair, area].astype(jnp.float32)
        y_copy(deep - 1, part).wait_recv()
        total = (total + y_in[deep - 1, area].astype(jnp.float32)) / root
        if part == 0:
            gu_ref[lower] = total
        else:
            gu_ref[other] = total[:main]
            gu_ref[middle] = total[main:]

    swap_copy().wait_send()
    rest_y().wait_send()
    for slot, (src_t, tp) in enumerate(((t, t_core), (t, t_x), (t_x, t_core))):
        cot_copy(src_t, slot, tp).wait_send()
    for k in range(2):
        forward_down(f, k, (-1, 1), finish)
        down_c(f_y, k).wait_send()
    for m in range(1, deep):
        if m < 3:
            up_z(m).wait_send()
            rest_z(m).wait_send()
        up_y(far(m)).wait_send()

    @pl.when(is_mid)
    def _():
        up_z(3).wait_send()
        rest_z(3).wait_send()
        relay_up().wait_send()
        relay_rest().wait_send()

    up_y(f).wait_send()
    for d in range(1, deep):
        for sign in (-1, 1):
            @pl.when(inside(z + sign * d))
            def _():
                src = f + 2 * sign * d
                for k in range(2):
                    forward_down(src, k, (-sign,), finish)
                    down_c(f_y + 2 * sign * d, k).wait_send()

    def drain(src, carry):
        grad_x(src).wait_send()
        grad_c(src).wait_send()
        return carry

    lax.fori_loop(0, n, drain, 0)
    for part in range(2):
        for pair in range(deep):
            y_copy(pair, part).wait_send()
            if pair < deep - 1:
                z_copy(pair, part).wait_send()


def settle(gi_ref, gu_ref, gi_out, gu_out):
    gi_out[...] = gi_ref[...]
    gu_out[...] = gu_ref[...]


def fused(n, tp, cotangent, inputs, pre_act, w_up, w_down):
    tokens, width = cotangent.shape
    rows = w_down.shape[0]
    own_rows = (rows - MIDDLE) // 2 + MIDDLE
    deep = n // 2
    dma = pltpu.SemaphoreType.DMA
    vmem = pl.BlockSpec(memory_space=pltpu.VMEM)
    anywhere = pl.BlockSpec(memory_space=pl.ANY)
    shapes = (
        jax.ShapeDtypeStruct((tokens, width), jnp.bfloat16),
        jax.ShapeDtypeStruct((rows, width), jnp.float32),
    )
    results = pl.pallas_call(
        functools.partial(kernel, n, tokens * n),
        out_shape=shapes,
        in_specs=[anywhere] * 5,
        out_specs=(vmem, vmem),
        scratch_shapes=[
            pltpu.VMEM((tokens, tp * width), jnp.bfloat16),
            pltpu.VMEM((tp * width, tokens), jnp.bfloat16),
            pltpu.VMEM((tokens, width), jnp.bfloat16),
            pltpu.VMEM((n, own_rows, tp * width), jnp.bfloat16),
            pltpu.VMEM((own_rows, width), jnp.bfloat16),
            pltpu.VMEM((n, rows, width), jnp.bfloat16),
            pltpu.VMEM((n, own_rows, tokens), jnp.bfloat16),
            pltpu.VMEM((n, rows, tokens), jnp.bfloat16),
            pltpu.VMEM((deep, rows, width), jnp.float32),
            pltpu.VMEM((deep, rows, width), jnp.bfloat16),
            pltpu.VMEM((deep, rows, width), jnp.bfloat16),
            pltpu.VMEM((deep - 1, rows, width), jnp.bfloat16),
            pltpu.VMEM((deep - 1, rows, width), jnp.bfloat16),
            dma((11,)),
            dma((3,)), dma((tp,)), dma((1,)),
            dma((2, deep, 2)), dma((deep, 2)), dma((n, 2)), dma((n, tp)),
            dma((deep,)), dma((deep + 1,)), dma((n,)), dma((deep,)), dma((n,)),
            dma((n,)), dma((n,)), dma((n,)), dma((n,)),
            dma((deep, 2)), dma((deep, 2)), dma((deep - 1, 2)), dma((deep - 1, 2)),
        ],
        compiler_params=pltpu.CompilerParams(
            collective_id=0, has_side_effects=True, vmem_limit_bytes=60 * 2**20
        ),
    )(cotangent, inputs, pre_act.T.reshape(n, rows, tokens), w_up, w_down)
    return pl.pallas_call(
        settle, out_shape=shapes, in_specs=[vmem, vmem], out_specs=(vmem, vmem)
    )(*results)


def gathered(cotangent, inputs, pre_act, w_up, w_down):
    token_total = cotangent.shape[0] * lax.axis_size("fs")
    full_cotangent = lax.all_gather(cotangent, "tp", axis=1, tiled=True)
    down_whole = lax.all_gather(w_down, "tp", axis=1, tiled=True)
    grad_hidden = times_rows(full_cotangent, lax.all_gather(down_whole, "fs", axis=0, tiled=True))
    grad_pre = (2.0 * grad_hidden * jnp.maximum(pre_act.astype(jnp.float32), 0.0)).astype(
        jnp.bfloat16
    )
    grad_input = jnp.dot(
        grad_pre, lax.all_gather(w_up, "fs", axis=0, tiled=True), preferred_element_type=jnp.float32
    )
    grad_share = lax.psum_scatter(
        lax.dot_general(
            grad_pre, inputs, (((0,), (0,)), ((), ())), preferred_element_type=jnp.float32
        ),
        "fs",
        scatter_dimension=0,
        tiled=True,
    )
    grad_up = grad_share / jnp.sqrt(jnp.float32(token_total))
    return (grad_input.astype(jnp.bfloat16), grad_up)


def solution(mesh):
    n, tp = mesh.shape["fs"], mesh.shape["tp"]

    def local(cotangent, inputs, pre_act, w_up, w_down):
        rows, width = w_down.shape
        fits = tp == 4 and n == 8 and rows % 128 == MIDDLE and width % 128 == 0
        if fits:
            return fused(n, tp, cotangent, inputs, pre_act, w_up, w_down)
        return gathered(cotangent, inputs, pre_act, w_up, w_down)

    return jax.shard_map(
        local,
        mesh=mesh,
        in_specs=(P("fs", "tp"), P("fs", "tp"), P("fs", None), P("fs", "tp"), P("fs", "tp")),
        out_specs=(P("fs", "tp"), P("fs", "tp")),
        check_vma=False,
    )
```

```python
import functools

import jax
import jax.numpy as jnp
from jax import lax
from jax.experimental import pallas as pl
from jax.experimental.pallas import tpu as pltpu
from jax.sharding import PartitionSpec as P

MESH = pl.DeviceIdType.MESH
MIDDLE = 8
ORDER = (
    ("uz", 1), ("rest",), ("cots",), ("line", 1, 0), ("core",), ("own",), ("rz", 3),
    ("line", 3, 0), ("line", 2, 0), ("line", 1, 1), ("uz", 3), ("rz", 2), ("cot",),
    ("line", 3, 1), ("uz", 2), ("line", 2, 1), ("beside", 0, 1), ("both",), ("beside", 0, 0),
    ("beside", 2, 0), ("make", 1), ("make", 6), ("beside", 1, 1), ("beside", 1, 0), ("make", 0),
    ("beside", 3, 0), ("beside", 3, 1), ("make", 4), ("beside", 2, 1), ("ufy", 1), ("rz", 1),
    ("make", 2), ("make", 3), ("make", 5), ("comb", 0, 0), ("gx", 1), ("comb", 2, 0), ("gx", 6),
    ("up",), ("gx", 0), ("make", 7), ("gx", 4), ("rrel",), ("more", 0), ("comb", 1, 0),
    ("gx", 2), ("more", 4), ("gx", 3), ("more", 1), ("more", 2), ("ufy", 2), ("more", 3),
    ("urel",), ("comb", 0, 1), ("gx", 5), ("ufy", 3), ("more", 5), ("comb", 2, 1), ("gx", 7),
    ("comb", 1, 1), ("more", 6), ("more", 7),
)


def times_rows(left, piece):
    return lax.dot_general(
        left, piece, (((1,), (1,)), ((), ())), preferred_element_type=jnp.float32
    )


def toggled(index, mask, bits):
    for bit in range(bits):
        unit = 2**bit
        index = index + unit * ((mask // unit) % 2) * (1 - 2 * ((index // unit) % 2))
    return index


def kernel(
    n, token_total,
    cot_hbm, in_hbm, pre_hbm, up_hbm, down_hbm,
    gi_ref, gu_ref,
    cot_buf, cot_turned, in_buf, down_buf, swap_buf, up_buf, pre_buf, grad, held,
    y_out, y_in, z_out, z_in,
    local_sem, cot_send, cot_recv, swap_send, dz_send, dy_send, dc_send, down_recv,
    uz_send, uy_send, up_recv, rest_send, rest_recv, gx_send, gx_recv, gc_send, gc_recv,
    ys_send, ys_recv, zs_send, zs_recv,
):
    deep = n // 2
    bits = n.bit_length() - 1
    f = lax.axis_index("fs")
    t = lax.axis_index("tp")
    z, y = f // 2, f % 2
    x, c = t // 2, t % 2
    width = in_buf.shape[1]
    rows = up_buf.shape[1]
    main = (rows - MIDDLE) // 2
    half = main // 2
    own_rows = main + MIDDLE
    t_core = t + 1 - 2 * c
    t_x = t + 2 - 4 * x
    t_xcore = t_core + 2 - 4 * x
    f_y = f + 1 - 2 * y
    is_mid = (z > 0) & (z < deep - 1)

    def cols(tp):
        return pl.ds(pl.multiple_of(tp * width, width), width)

    def far(m):
        return toggled(f, 2 * m, bits)

    def seq(i):
        pair = i // 2
        return toggled(f, 2 * ((pair + 1) % deep) + (i + 1) % 2, bits)

    def remote(src, dst, send, recv, fs, tp):
        return pltpu.make_async_remote_copy(
            src_ref=src, dst_ref=dst, send_sem=send, recv_sem=recv,
            device_id=(fs, tp), device_id_type=MESH,
        )

    lower = pl.ds(pl.multiple_of((main + MIDDLE) * x, 8), main)
    other = pl.ds(pl.multiple_of((main + MIDDLE) * (1 - x), 8), main)
    middle = pl.ds(main, MIDDLE)
    first, second, last = pl.ds(0, main), pl.ds(main, main), pl.ds(2 * main, MIDDLE)
    parts = (first, pl.ds(main, own_rows))

    plan = [
        (down_hbm.at[other], swap_buf.at[first]),
        (down_hbm.at[middle], swap_buf.at[middle]),
        (down_hbm.at[lower], down_buf.at[f, first, cols(t)]),
        (down_hbm.at[middle], down_buf.at[f, middle, cols(t)]),
        (cot_hbm, cot_buf.at[:, cols(t)]),
        (up_hbm.at[lower], up_buf.at[f, first]),
        (up_hbm.at[other], up_buf.at[f, second]),
        (up_hbm.at[middle], up_buf.at[f, last]),
        (in_hbm, in_buf),
        (pre_hbm.at[:, lower], pre_buf.at[:, first]),
        (pre_hbm.at[:, middle], pre_buf.at[:, middle]),
    ]
    local = [
        pltpu.make_async_copy(src, dst, local_sem.at[k]) for k, (src, dst) in enumerate(plan)
    ]
    for copy in local:
        copy.start()

    def swap_copy():
        return remote(
            swap_buf, down_buf.at[f, :, cols(t)], swap_send.at[0], down_recv.at[f, t], f, t_x
        )

    def cot_copy(src_t, slot, tp):
        block = cot_buf.at[:, cols(src_t)]
        return remote(block, block, cot_send.at[slot], cot_recv.at[src_t], f, tp)

    def piece(k):
        return t if k == 0 else t_x

    def down_copy(src_f, k, send, fs, tp):
        block = down_buf.at[src_f, :, cols(piece(k))]
        return remote(block, block, send, down_recv.at[src_f, piece(k)], fs, tp)

    def down_z(src_f, k, step):
        return down_copy(src_f, k, dz_send.at[(1 + step) // 2, src_f // 2, k], f + 2 * step, t)

    def down_y(src_f, k):
        return down_copy(src_f, k, dy_send.at[src_f // 2, k], f_y, t)

    def down_c(src_f, k):
        return down_copy(src_f, k, dc_send.at[src_f, k], f, t_core)

    def up_copy(src_f, area, send, recv, fs):
        block = up_buf.at[src_f, area]
        return remote(block, block, send, recv.at[src_f], fs, t)

    def up_z(m):
        return up_copy(f, pl.ds(0, rows), uz_send.at[m], up_recv, far(m))

    def rest_z(m):
        return up_copy(f_y, parts[1], rest_send.at[m], rest_recv, far(m))

    def up_y(src_f):
        return up_copy(src_f, parts[0], uy_send.at[src_f // 2], up_recv, f_y)

    def rest_y():
        return up_copy(f, parts[1], uy_send.at[deep], rest_recv, f_y)

    def grad_x(src_f):
        src = grad.at[src_f, pl.ds(pl.multiple_of(half * c, half), half)]
        dst = grad.at[src_f, pl.ds(pl.multiple_of(main + half * c, half), half)]
        return remote(src, dst, gx_send.at[src_f], gx_recv.at[src_f], f, t_x)

    def grad_c(src_f):
        block = grad.at[src_f, pl.ds(pl.multiple_of(main + half * c, half), half)]
        return remote(block, block, gc_send.at[src_f], gc_recv.at[src_f], f, t_core)

    def y_copy(pair, part):
        return remote(
            y_out.at[pair, parts[part]], y_in.at[pair, parts[part]],
            ys_send.at[pair, part], ys_recv.at[pair, part], f_y, t,
        )

    def z_copy(pair, part):
        return remote(
            z_out.at[pair, parts[part]], z_in.at[pair, parts[part]],
            zs_send.at[pair, part], zs_recv.at[pair, part], far(pair + 1), t,
        )

    def inside(zz):
        return (zz >= 0) & (zz < deep)

    barrier = pltpu.get_barrier_semaphore()
    for peer in ((f_y, t), (f, t_core), (f, t_x)):
        pl.semaphore_signal(barrier, inc=1, device_id=peer, device_id_type=MESH)
    for step in (-1, 1):
        @pl.when(inside(z + step))
        def _():
            pl.semaphore_signal(barrier, inc=1, device_id=(f + 2 * step, t), device_id_type=MESH)

    for k in range(8):
        local[k].wait()
    pl.semaphore_wait(barrier, 4 + is_mid.astype(jnp.int32))

    def arrived_down(src_f, tp):
        block = down_buf.at[src_f, :, cols(tp)]
        remote(block, block, swap_send.at[0], down_recv.at[src_f, tp], f, t_core).wait_recv()

    def arrived_cot(src_t):
        cot_copy(src_t, 0, t_core).wait_recv()

    def forward_down(src_f, k, steps, act):
        for step in steps:
            @pl.when(inside(z + step))
            def _():
                act(down_z(src_f, k, step))
        act(down_y(src_f, k))
        act(down_c(src_f, k))

    def start(copy):
        copy.start()

    def finish(copy):
        copy.wait_send()

    def arrived_up(src_f):
        up_copy(src_f, pl.ds(0, rows), uz_send.at[0], up_recv, f_y).wait_recv()

    def arrived_rest(src_f):
        up_copy(src_f, parts[1], uy_send.at[deep], rest_recv, f_y).wait_recv()

    def turn(tp):
        cot_turned[cols(tp)] = cot_buf[:, cols(tp)].T

    def share(pair, part, across, value):
        if across:
            y_out[pair, parts[part]] = value.astype(jnp.bfloat16)
            y_copy(pair, part).start()
        else:
            held[pair, parts[part]] = value

    def relay_up():
        return up_copy(far(2), pl.ds(0, rows), uz_send.at[0], up_recv, far(1))

    def relay_rest():
        return up_copy(toggled(f, 5, bits), parts[1], rest_send.at[0], rest_recv, far(1))

    seen = set()

    def once(name, act):
        if name not in seen:
            seen.add(name)
            act()

    def do_own():
        arrived_down(f, t_x)
        forward_down(f, 1, (-1, 1), start)

    def do_line(m, k):
        src = far(m)
        arrived_down(src, piece(k))
        for step in (-1, 1):
            @pl.when(inside(z + step) & ((src < f) == (step > 0)))
            def _():
                down_z(src, k, step).start()

        down_y(src, k).start()
        down_c(src, k).start()

    def do_beside(m, k):
        src = toggled(f, 2 * m + 1, bits)
        arrived_down(src, piece(k))
        down_c(src, k).start()

    def do_cots():
        cot_copy(t, 1, t_x).start()
        cot_copy(t, 0, t_core).start()
        turn(t)

    def do_cot_core():
        arrived_cot(t_core)
        turn(t_core)

    def do_cot_x():
        arrived_cot(t_x)
        cot_copy(t_x, 2, t_core).start()
        turn(t_x)

    def do_cot_xc():
        arrived_cot(t_xcore)
        turn(t_xcore)

    def do_uz(m):
        if m < 3:
            up_z(m).start()
        else:
            @pl.when(is_mid)
            def _():
                up_z(3).start()

    def do_rz(m):
        once("rest", lambda: arrived_rest(f_y))
        if m < 3:
            rest_z(m).start()
        else:
            @pl.when(is_mid)
            def _():
                rest_z(3).start()

    def do_ufy(m):
        once(("up", m), lambda: arrived_up(far(m)))
        up_y(far(m)).start()

    def do_urel():
        once(("up", 2), lambda: arrived_up(far(2)))

        @pl.when(is_mid)
        def _():
            relay_up().start()

    def do_rrel():
        @pl.when(is_mid)
        def _():
            relay_rest().wait_recv()
            relay_rest().start()

    def more_local():
        for k in range(8, len(local)):
            local[k].wait()

    def do_make(i):
        once("local", more_local)
        src = seq(i)
        arrived_down(src, t_core)
        arrived_down(src, t_xcore)
        hidden = jnp.dot(down_buf[src], cot_turned[...], preferred_element_type=jnp.float32)
        grad_pre = (
            2.0 * hidden * jnp.maximum(pre_buf[src].astype(jnp.float32), 0.0)
        ).astype(jnp.bfloat16)
        grad[src, first] = grad_pre[:main]
        grad[src, last] = grad_pre[main:]
        grad_x(src).start()
        share(i // 2, 0, i % 2 == 0, jnp.dot(
            grad_pre[:main], in_buf[...], preferred_element_type=jnp.float32
        ))

    def do_gx(i):
        src = seq(i)
        grad_x(src).wait_recv()
        grad_c(src).start()

    def do_more(i):
        src = seq(i)
        grad_c(src).wait_recv()
        share(i // 2, 1, i % 2 == 0, jnp.dot(
            grad[src, parts[1]], in_buf[...], preferred_element_type=jnp.float32
        ))

    def do_comb(pair, part):
        y_copy(pair, part).wait_recv()
        area = parts[part]
        z_out[pair, area] = (
            held[pair, area] + y_in[pair, area].astype(jnp.float32)
        ).astype(jnp.bfloat16)
        z_copy(pair, part).start()

    swap_copy().start()
    forward_down(f, 0, (-1, 1), start)
    acts = {
        "own": do_own, "line": do_line, "beside": do_beside, "cots": do_cots,
        "core": do_cot_core, "cot": do_cot_x, "both": do_cot_xc,
        "rest": lambda: rest_y().start(), "up": lambda: up_y(f).start(),
        "uz": do_uz, "rz": do_rz, "ufy": do_ufy, "urel": do_urel, "rrel": do_rrel,
        "make": do_make, "gx": do_gx, "more": do_more, "comb": do_comb,
    }
    for name, *values in ORDER:
        acts[name](*values)

    for m in range(deep):
        src = toggled(f, 2 * m + 1, bits)
        up_y(src).wait_recv()
        rest = up_copy(src, parts[1], uy_send.at[deep], rest_recv, f_y)
        if m == 2:
            @pl.when(jnp.logical_not(is_mid))
            def _():
                rest.wait_recv()
        elif m:
            rest.wait_recv()
    gi = jnp.zeros(gi_ref.shape, jnp.float32)
    for block in range(n):
        gi = gi + lax.dot_general(
            grad[block], up_buf[block], (((0,), (0,)), ((), ())),
            preferred_element_type=jnp.float32,
        )
    gi_ref[...] = gi.astype(gi_ref.dtype)

    root = jnp.sqrt(jnp.float32(token_total))
    for part, area in enumerate(parts):
        total = held[deep - 1, area]
        for pair in range(deep - 1):
            z_copy(pair, part).wait_recv()
            total = total + z_in[pair, area].astype(jnp.float32)
        y_copy(deep - 1, part).wait_recv()
        total = (total + y_in[deep - 1, area].astype(jnp.float32)) / root
        if part == 0:
            gu_ref[lower] = total
        else:
            gu_ref[other] = total[:main]
            gu_ref[middle] = total[main:]

    swap_copy().wait_send()
    rest_y().wait_send()
    for slot, (src_t, tp) in enumerate(((t, t_core), (t, t_x), (t_x, t_core))):
        cot_copy(src_t, slot, tp).wait_send()
    for k in range(2):
        forward_down(f, k, (-1, 1), finish)
        down_c(f_y, k).wait_send()
    for m in range(1, deep):
        if m < 3:
            up_z(m).wait_send()
            rest_z(m).wait_send()
        up_y(far(m)).wait_send()

    @pl.when(is_mid)
    def _():
        up_z(3).wait_send()
        rest_z(3).wait_send()
        relay_up().wait_send()
        relay_rest().wait_send()

    up_y(f).wait_send()
    for d in range(1, deep):
        for sign in (-1, 1):
            @pl.when(inside(z + sign * d))
            def _():
                src = f + 2 * sign * d
                for k in range(2):
                    forward_down(src, k, (-sign,), finish)
                    down_c(f_y + 2 * sign * d, k).wait_send()

    def drain(src, carry):
        grad_x(src).wait_send()
        grad_c(src).wait_send()
        return carry

    lax.fori_loop(0, n, drain, 0)
    for part in range(2):
        for pair in range(deep):
            y_copy(pair, part).wait_send()
            if pair < deep - 1:
                z_copy(pair, part).wait_send()


def settle(gi_ref, gu_ref, gi_out, gu_out):
    gi_out[...] = gi_ref[...]
    gu_out[...] = gu_ref[...]


def fused(n, tp, cotangent, inputs, pre_act, w_up, w_down):
    tokens, width = cotangent.shape
    rows = w_down.shape[0]
    own_rows = (rows - MIDDLE) // 2 + MIDDLE
    deep = n // 2
    dma = pltpu.SemaphoreType.DMA
    vmem = pl.BlockSpec(memory_space=pltpu.VMEM)
    anywhere = pl.BlockSpec(memory_space=pltpu.HBM)
    shapes = (
        jax.ShapeDtypeStruct((tokens, width), jnp.bfloat16),
        jax.ShapeDtypeStruct((rows, width), jnp.float32),
    )
    results = pl.pallas_call(
        functools.partial(kernel, n, tokens * n),
        out_shape=shapes,
        in_specs=[anywhere] * 5,
        out_specs=(vmem, vmem),
        scratch_shapes=[
            pltpu.VMEM((tokens, tp * width), jnp.bfloat16),
            pltpu.VMEM((tp * width, tokens), jnp.bfloat16),
            pltpu.VMEM((tokens, width), jnp.bfloat16),
            pltpu.VMEM((n, own_rows, tp * width), jnp.bfloat16),
            pltpu.VMEM((own_rows, width), jnp.bfloat16),
            pltpu.VMEM((n, rows, width), jnp.bfloat16),
            pltpu.VMEM((n, own_rows, tokens), jnp.bfloat16),
            pltpu.VMEM((n, rows, tokens), jnp.bfloat16),
            pltpu.VMEM((deep, rows, width), jnp.float32),
            pltpu.VMEM((deep, rows, width), jnp.bfloat16),
            pltpu.VMEM((deep, rows, width), jnp.bfloat16),
            pltpu.VMEM((deep - 1, rows, width), jnp.bfloat16),
            pltpu.VMEM((deep - 1, rows, width), jnp.bfloat16),
            dma((11,)),
            dma((3,)), dma((tp,)), dma((1,)),
            dma((2, deep, 2)), dma((deep, 2)), dma((n, 2)), dma((n, tp)),
            dma((deep,)), dma((deep + 1,)), dma((n,)), dma((deep,)), dma((n,)),
            dma((n,)), dma((n,)), dma((n,)), dma((n,)),
            dma((deep, 2)), dma((deep, 2)), dma((deep - 1, 2)), dma((deep - 1, 2)),
        ],
        compiler_params=pltpu.CompilerParams(
            collective_id=0, has_side_effects=True, vmem_limit_bytes=24 * 2**20
        ),
    )(*(pltpu.with_memory_space_constraint(q, pltpu.HBM) for q in (cotangent, inputs, pre_act.T.reshape(n, rows, tokens), w_up, w_down)))
    return pl.pallas_call(
        settle, out_shape=shapes, in_specs=[vmem, vmem], out_specs=(vmem, vmem),
        compiler_params=pltpu.CompilerParams(vmem_limit_bytes=4 * 2**20),
    )(*results)


def gathered(cotangent, inputs, pre_act, w_up, w_down):
    token_total = cotangent.shape[0] * lax.axis_size("fs")
    full_cotangent = lax.all_gather(cotangent, "tp", axis=1, tiled=True)
    down_whole = lax.all_gather(w_down, "tp", axis=1, tiled=True)
    grad_hidden = times_rows(full_cotangent, lax.all_gather(down_whole, "fs", axis=0, tiled=True))
    grad_pre = (2.0 * grad_hidden * jnp.maximum(pre_act.astype(jnp.float32), 0.0)).astype(
        jnp.bfloat16
    )
    grad_input = jnp.dot(
        grad_pre, lax.all_gather(w_up, "fs", axis=0, tiled=True), preferred_element_type=jnp.float32
    )
    grad_share = lax.psum_scatter(
        lax.dot_general(
            grad_pre, inputs, (((0,), (0,)), ((), ())), preferred_element_type=jnp.float32
        ),
        "fs",
        scatter_dimension=0,
        tiled=True,
    )
    grad_up = grad_share / jnp.sqrt(jnp.float32(token_total))
    return (grad_input.astype(jnp.bfloat16), grad_up)


def solution(mesh):
    n, tp = mesh.shape["fs"], mesh.shape["tp"]

    def local(cotangent, inputs, pre_act, w_up, w_down):
        rows, width = w_down.shape
        fits = tp == 4 and n == 8 and rows % 128 == MIDDLE and width % 128 == 0
        if fits:
            return fused(n, tp, cotangent, inputs, pre_act, w_up, w_down)
        return gathered(cotangent, inputs, pre_act, w_up, w_down)

    return jax.shard_map(
        local,
        mesh=mesh,
        in_specs=(P("fs", "tp"), P("fs", "tp"), P("fs", None), P("fs", "tp"), P("fs", "tp")),
        out_specs=(P("fs", "tp"), P("fs", "tp")),
        check_vma=False,
    )
```
